32 devices in a mesh: grp: 2 (over y), sp: 4 (over z), tp: 4 (over x, core).
Axes of the slice: x: 2, y: 2, z: 4, core: 2. Of those that a mesh axis runs over, the one named last changes fastest.
Arguments:
- tokens: bfloat16 [16384, 2048], P(('grp', 'sp')), parts along dimension 0, may hold values from -6 to 6
- in_gain: float32 [2048], replicated, may hold values from 0.1 to 1.9
- w_input: bfloat16 [2048, 2048], P(None, 'tp'), may hold values from -0.125 to 0.125
- w_gate: bfloat16 [2048, 2048], P(None, 'tp'), may hold values from -4 to 4
- conv_taps: float32 [4, 2048], P(None, 'tp'), may hold values from -3 to 3
- w_rate: bfloat16 [8, 256, 256], P('tp'), may hold values from -0.375 to 0.375
- w_inlet: bfloat16 [8, 256, 256], P('tp'), may hold values from -0.375 to 0.375
- decay_param: float32 [2048], P('tp'), may hold values from 3 to 25
- decay_bias: float32 [8, 16384], P('tp', ('grp', 'sp')), parts along dimension 1, may hold values from -1.5 to 0
- out_gain: float32 [2048], P('tp'), may hold values from 0.1 to 1.9
- w_out: bfloat16 [2048, 2048], P('sp'), may hold values from -0.125 to 0.125
Outputs:
- mixer_out: bfloat16 [16384, 2048], P(('grp', 'sp', 'tp')), parts along dimension 0
The draws below stay inside these ranges and needn't reach their ends.
There are 2 independent parts, one for each index of `grp`. The reference program is written for one: setup_inputs(seed, part) draws one part's arguments, and reference() takes and returns one part's arrays. A program takes and returns all parts, laid end to end along the dimension named above; an argument that names none is the same for every part. Nothing has to cross between parts.
All inputs are finite; a program needn't handle non-finite values.
Results may differ from the reference program's by a relative error of at most 0.013.
Values may be sent and summed in bfloat16 or wider, within the bound.
A program may use at most 128 MiB of HBM per device.

```python
import math
import jax
import jax.numpy as jnp
from jax import lax

D = 2048
HEADS = 8
HEAD = 256
CONV = 4
SEQ_DEV = 2048
DR = 2048
SEQ = 8192


def draw_w_gate(key, part):
    base_key, jitter_key = jax.random.split(jax.random.fold_in(key, 11))
    columns = HEADS * HEAD
    base = jnp.clip(jax.random.normal(base_key, (D, columns), jnp.float32), -4.0, 4.0)
    position = jnp.arange(columns, dtype=jnp.float32) / columns
    jitter = jax.random.uniform(jitter_key, (columns,), jnp.float32) / HEADS
    column_scale = jnp.exp((position + jitter) * math.log(6.0))
    return (base * column_scale[None, :] / math.sqrt(D)).astype(jnp.bfloat16)


def draw_decay_param(key, part):
    pick_key, slow_key, fast_key = jax.random.split(jax.random.fold_in(key, 23), 3)
    channels = HEADS * HEAD
    slow = jax.random.bernoulli(pick_key, 0.5, (channels,))
    slow_rate = jax.random.uniform(slow_key, (channels,), jnp.float32, 0.2, 0.6) / (8.0 * SEQ)
    fast_rate = jnp.exp(jax.random.uniform(fast_key, (channels,), jnp.float32, math.log(1.0 / 400.0), math.log(1.0 / 120.0)))
    chosen = jnp.where(slow, slow_rate, fast_rate)
    return -jnp.log(jnp.expm1(chosen))


def draw_decay_bias(key, part):
    span_key, spot_key, depth_key = jax.random.split(jax.random.fold_in(key, 37), 3)
    span_count = SEQ // SEQ_DEV
    level = jnp.exp(jax.random.uniform(span_key, (HEADS, span_count), jnp.float32, math.log(0.2), math.log(1.2))) / SEQ
    dispersion = jnp.repeat(-level, SEQ_DEV, axis=1)
    spots = jax.random.randint(spot_key, (HEADS, 2), 0, SEQ)
    layer_count = jnp.log(jax.random.uniform(depth_key, (HEADS, 2), jnp.float32, 0.55, 0.8))
    match_count = (jnp.arange(SEQ, dtype=jnp.int32)[None, None, :] == spots[:, :, None]).astype(jnp.float32)
    pulse_train = jnp.sum(match_count * layer_count[:, :, None], axis=1)
    return dispersion + pulse_train


def level_of(key, dims, shards, least, top_value):
    factor_of = 1.0
    for dim, parts in shards:
        heights = jax.random.uniform(jax.random.fold_in(jax.random.fold_in(key, 6), dim), (parts,), jnp.float32, least / len(shards), top_value / len(shards))
        factor_of = factor_of * jnp.repeat(jnp.exp(heights), dims[dim] // parts).reshape((-1,) + (1,) * (len(dims) - 1 - dim))
    return factor_of


def scatter_about(key, dims, deviation, reach, shards=(), held_as=jnp.bfloat16):
    factor_of = level_of(key, dims, shards, -0.22, 0.18) if shards else 1.0
    drawn = jax.random.normal(key, dims, jnp.float32) * deviation * factor_of
    return jnp.minimum(jnp.maximum(drawn, -reach), reach).astype(held_as)


def setup_inputs(seed: int = 0, part: int = 0) -> dict:
    key_of = jax.random.split(jax.random.key(seed), 12)
    own_keys = jax.random.split(jax.random.fold_in(key_of[11], part), 12)
    return {
        "tokens": scatter_about(own_keys[0], (SEQ, D), 1.0, 6.0, ((0, 4),)),
        "in_gain": jnp.clip(1.0 + 0.18 * jax.random.normal(key_of[1], (D,), jnp.float32), 0.1, 1.9),
        "w_input": scatter_about(key_of[2], (D, DR), D ** -0.5, 0.125, ((1, 4),)),
        "w_gate": draw_w_gate(jax.random.fold_in(key_of[11], 71), part),
        "conv_taps": scatter_about(key_of[4], (CONV, DR), 0.5, 3.0, ((1, 4),), jnp.float32),
        "w_rate": scatter_about(key_of[5], (HEADS, HEAD, HEAD), HEAD ** -0.5, 0.375, ((0, 4),)),
        "w_inlet": scatter_about(key_of[6], (HEADS, HEAD, HEAD), HEAD ** -0.5, 0.375, ((0, 4),)),
        "decay_param": draw_decay_param(jax.random.fold_in(key_of[11], 71), part),
        "decay_bias": draw_decay_bias(jax.random.fold_in(jax.random.fold_in(key_of[11], part), 71), part),
        "out_gain": jnp.clip(1.0 + 0.18 * jax.random.normal(key_of[9], (DR,), jnp.float32), 0.1, 1.9),
        "w_out": scatter_about(key_of[10], (DR, D), DR ** -0.5, 0.125, ((0, 4),)),
    }


def combine_pairs(first_pair, second_pair):
    return (first_pair[0] * second_pair[0], second_pair[0] * first_pair[1] + second_pair[1])

def reference(tokens, in_gain, w_input, w_gate, conv_taps, w_rate, w_inlet, decay_param, decay_bias, out_gain, w_out):
    seq_len = tokens.shape[0]
    as_float = tokens.astype(jnp.float32)
    inv_norm = lax.rsqrt(lax.optimization_barrier(jnp.mean(as_float * as_float, axis=1, keepdims=True)) + 1e-06)
    normed = (as_float * inv_norm * in_gain).astype(jnp.bfloat16)
    projected = jnp.dot(normed, w_input, preferred_element_type=jnp.float32).astype(jnp.bfloat16)
    gate_raw = jnp.dot(normed, w_gate, preferred_element_type=jnp.float32).astype(jnp.bfloat16)
    padded = jnp.pad(projected.astype(jnp.float32), ((CONV - 1, 0), (0, 0)))
    tap_values = conv_taps.astype(jnp.float32)
    summed = padded[0:seq_len] * tap_values[0]
    for offset in range(1, CONV):
        summed = summed + padded[offset:offset + seq_len] * tap_values[offset]
    convolved = summed.astype(jnp.bfloat16)
    per_head = convolved.astype(jnp.float32).reshape(seq_len, HEADS, HEAD)
    rate_gate = jax.nn.sigmoid(jnp.einsum('shi,hij->shj', per_head, w_rate.astype(jnp.float32))).reshape(seq_len, HEADS * HEAD)
    input_gate = jax.nn.sigmoid(jnp.einsum('shi,hij->shj', per_head, w_inlet.astype(jnp.float32))).reshape(seq_len, HEADS * HEAD)
    head_bias = jnp.repeat(jnp.transpose(decay_bias), HEAD, axis=1)
    log_decay = -8.0 * rate_gate * jax.nn.softplus(-decay_param) + head_bias
    drive_term = jnp.sqrt(-jnp.expm1(2.0 * log_decay)) * input_gate * convolved.astype(jnp.float32)
    decay_prod, full_state = lax.associative_scan(combine_pairs, (jnp.exp(log_decay), drive_term), axis=0)
    gated_out = full_state * jax.nn.gelu(gate_raw.astype(jnp.float32))
    out_scale = lax.rsqrt(lax.optimization_barrier(jnp.mean(gated_out * gated_out, axis=1, keepdims=True)) + 1e-06)
    normed_out = (gated_out * out_scale * out_gain).astype(jnp.bfloat16)
    return jnp.dot(normed_out, w_out, preferred_element_type=jnp.float32).astype(jnp.bfloat16)
```

```python
import functools
import jax
import jax.numpy as jnp
from jax import lax
from jax.experimental import pallas as pl
from jax.experimental.pallas import tpu as pltpu
from jax.sharding import PartitionSpec as P

MESH = pl.DeviceIdType.MESH
F32 = jnp.float32
BF16 = jnp.bfloat16
CHUNK = 256
SUB = 32


def normalize(raw, gain):
    as_float = raw.astype(F32)
    inv = lax.rsqrt(jnp.mean(as_float * as_float, axis=1, keepdims=True) + 1e-06)
    return (as_float * inv * gain).astype(BF16)


def one_minus_square(log_decay, decay):
    y = 2.0 * log_decay
    series = -y * (1.0 + y * (0.5 + y * (1.0 / 6 + y * (1.0 / 24 + y * (1.0 / 120)))))
    return jnp.where(y > -0.1, series, 1.0 - decay * decay)


def kernel(
    sizes,
    tokens, in_gain, w_input, w_gate, taps, w_rate, w_inlet, rate_scale, bias, out_gain, w_out,
    out,
    x, wi, wg, w_all, state, prod, gate, gated, arrived, total, result, halo, padded, conv,
    rate_in, inlet_in, squares, squares_in, ends, ends_in,
    x_sem, load_sem, halo_send, halo_recv, z_send, z_recv, y_send, y_recv, c_send, c_recv,
    end_send, end_recv, a_send, a_recv, q_send, q_recv, own_sem, out_sem,
):
    n_grp, n_sp, n_tp = sizes
    grp, sp, tp = lax.axis_index("grp"), lax.axis_index("sp"), lax.axis_index("tp")
    rows, width = tokens.shape
    heads, head = w_rate.shape[0], w_rate.shape[1]
    reach = taps.shape[0] - 1
    chunks = rows // CHUNK
    out_rows = rows // n_tp
    shard = w_out.shape[0]
    parts = n_grp * 2
    piece = shard // parts
    core = lax.rem(tp, 2)
    mate = tp + 1 - 2 * core
    across = 1 - grp
    quarter = grp * 2 + core
    quarter_across = across * 2 + core

    def x_copy(i):
        at = pl.ds(pl.multiple_of(i * CHUNK, CHUNK), CHUNK)
        return pltpu.make_async_copy(tokens.at[at], x.at[at], x_sem.at[i])

    loads = [
        pltpu.make_async_copy(w_input, wi, load_sem.at[0]),
        pltpu.make_async_copy(w_gate, wg, load_sem.at[1]),
        pltpu.make_async_copy(
            w_out, w_all.at[pl.ds(pl.multiple_of(sp * shard, shard), shard)], load_sem.at[2]
        ),
    ]
    loads[0].start()
    x_copy(0).start()
    loads[1].start()
    for i in range(1, chunks):
        x_copy(i).start()
    loads[2].start()

    barrier = pltpu.get_barrier_semaphore()
    for d in range(1, n_sp):
        pl.semaphore_signal(
            barrier, inc=1, device_id={"sp": lax.rem(sp + d, n_sp)}, device_id_type=MESH
        )
    for k in range(1, n_tp):
        pl.semaphore_signal(
            barrier, inc=1, device_id={"tp": lax.rem(tp + k, n_tp)}, device_id_type=MESH
        )
    pl.semaphore_signal(barrier, inc=1, device_id={"grp": across}, device_id_type=MESH)
    pl.semaphore_wait(barrier, n_sp - 1 + n_tp - 1 + 1)

    def remote(src, dst, send, recv, where):
        return pltpu.make_async_remote_copy(
            src_ref=src, dst_ref=dst, send_sem=send, recv_sem=recv,
            device_id=where, device_id_type=MESH,
        )

    halo_rows = halo.shape[0]
    halo_copy = remote(
        tokens.at[pl.ds(rows - halo_rows, halo_rows)], halo, halo_send, halo_recv,
        {"sp": lax.rem(sp + 1, n_sp)},
    )
    halo_copy.start()

    def w_rows(source, part):
        return w_all.at[pl.ds(pl.multiple_of(source * shard + part * piece, piece), piece)]

    def z_copy(d):
        return remote(
            w_out.at[pl.ds(pl.multiple_of(quarter * piece, piece), piece)],
            w_rows(sp, quarter), z_send.at[d], z_recv.at[d], {"sp": lax.rem(sp + d, n_sp)},
        )

    def y_copy(d):
        at = w_rows(lax.rem(sp + n_sp - d, n_sp), quarter)
        return remote(at, at, y_send.at[d], y_recv.at[d], {"grp": across})

    def c_copy(d, second):
        at = w_rows(
            lax.rem(sp + n_sp - d, n_sp), quarter_across if second else quarter
        )
        k = 2 * d + second
        return remote(at, at, c_send.at[k], c_recv.at[k], {"tp": mate})

    near = sorted({1, n_sp - 1})
    far = [d for d in range(2, n_sp - 1)]

    def forward_first(group):
        for d in group:
            z_copy(d).wait_recv()
            y_copy(d).start()
            c_copy(d, 0).start()

    def forward_second(group):
        for d in group:
            y_copy(d).wait_recv()
            c_copy(d, 1).start()

    for d in near:
        z_copy(d).start()

    gain_row = in_gain[...]
    sublane = lax.broadcasted_iota(jnp.int32, (SUB // 8, 8, head), 1)

    def lanes_of(h):
        return slice(h * head, (h + 1) * head)

    def spread(row):
        return jnp.broadcast_to(row, (8, row.shape[1]))

    def start_conv(h):
        before = normalize(halo[...], gain_row)
        before = jnp.dot(before, wi[:, lanes_of(h)], preferred_element_type=F32)
        before = before.astype(BF16).astype(F32)
        padded[0:8, :] = jnp.where(sp > 0, before[halo_rows - 8 :], 0.0)

    def phase_a(h, i, carry):
        lanes = lanes_of(h)
        at = pl.ds(pl.multiple_of(i * CHUNK, CHUNK), CHUNK)
        if h == 0:
            x_copy(i).wait()
            x[at, :] = normalize(x[at, :], gain_row)
        normed = x[at, :]
        projected = jnp.dot(normed, wi[:, lanes], preferred_element_type=F32)
        padded[8:, :] = projected.astype(BF16).astype(F32)
        for r in range(0, CHUNK, SUB):
            summed = padded[8 - reach + r : 8 - reach + r + SUB, :] * taps[0:1, lanes]
            for k in range(1, reach + 1):
                first = 8 - reach + k + r
                summed = summed + padded[first : first + SUB, :] * taps[k : k + 1, lanes]
            conv[r : r + SUB, :] = summed.astype(BF16)
        padded[0:8, :] = padded[CHUNK:, :]
        rate_in[...] = jnp.dot(conv[...], w_rate[h], preferred_element_type=F32)
        inlet_in[...] = jnp.dot(conv[...], w_inlet[h], preferred_element_type=F32)
        gate_raw = jnp.dot(normed, wg[:, lanes], preferred_element_type=F32)
        gate[at, lanes] = gate_raw
        bias_row = bias[h : h + 1, at]
        bias_cols = jnp.broadcast_to(bias_row, (128, CHUNK)).T
        scale = rate_scale[0:1, lanes]
        s, p = carry
        for r in range(0, CHUNK, SUB):
            here = slice(r, r + SUB)
            into = pl.ds(pl.multiple_of(i * CHUNK + r, SUB), SUB)
            raw = gate[into, lanes].astype(BF16).astype(F32)
            gate[into, lanes] = jax.nn.gelu(raw)
            bias_here = jnp.concatenate([bias_cols[here]] * (head // 128), axis=1)
            log_decay = jax.nn.sigmoid(rate_in[here, :]) * scale + bias_here
            decay = jnp.exp(log_decay)
            drive = (
                jnp.sqrt(one_minus_square(log_decay, decay))
                * jax.nn.sigmoid(inlet_in[here, :])
                * conv[here, :].astype(F32)
            )
            pt = decay.reshape(SUB // 8, 8, head)
            st = drive.reshape(SUB // 8, 8, head)
            for d in (1, 2, 4):
                inside = sublane >= d
                st = st + pt * jnp.where(inside, pltpu.roll(st, d, 1), 0.0)
                pt = pt * jnp.where(inside, pltpu.roll(pt, d, 1), 1.0)
            s_parts, p_parts = [], []
            for t in range(SUB // 8):
                s_parts.append(st[t] + pt[t] * s)
                p_parts.append(pt[t] * p)
                p_last = spread(pt[t, 7:8])
                s = spread(st[t, 7:8]) + p_last * s
                p = p_last * p
            state[into, lanes] = jnp.concatenate(s_parts, axis=0)
            prod[into, lanes] = jnp.concatenate(p_parts, axis=0)
        return s, p

    def start_carry():
        return jnp.zeros((8, head), F32), jnp.ones((8, head), F32)

    def end_copy(h, d):
        k = h * n_sp + d
        return remote(
            ends.at[h], ends_in.at[k], end_send.at[k], end_recv.at[k],
            {"sp": lax.rem(sp + d, n_sp)},
        )

    def send_ends(h, carry):
        s, p = carry
        ends[h, 0:8, :] = s
        ends[h, 8:16, :] = p
        for d in range(1, n_sp):
            end_copy(h, d).start()

    def take_ends(h):
        carry = jnp.zeros((8, head), F32)
        for d in range(n_sp - 1, 0, -1):
            end_copy(h, d).wait_recv()
            k = h * n_sp + d
            new = ends_in[k, 0:8, :] + ends_in[k, 8:16, :] * carry
            carry = jnp.where(d <= sp, new, carry)
        return carry[0:1]

    def a_copy(h, k):
        to = lax.rem(tp + k, n_tp)
        at = pl.ds(pl.multiple_of(to * out_rows, out_rows), out_rows)
        slot = h * n_tp + k
        return remote(
            gated.at[h, at], arrived.at[tp * heads + h], a_send.at[slot], a_recv.at[slot],
            {"tp": to},
        )

    def q_copy(h, k):
        to = lax.rem(tp + k, n_tp)
        slot = h * n_tp + k
        return remote(
            squares.at[h * n_tp + to], squares_in.at[tp * heads + h],
            q_send.at[slot], q_recv.at[slot], {"tp": to},
        )

    def own_copies(h):
        at = pl.ds(pl.multiple_of(tp * out_rows, out_rows), out_rows)
        return (
            pltpu.make_async_copy(gated.at[h, at], arrived.at[tp * heads + h], own_sem.at[2 * h]),
            pltpu.make_async_copy(
                squares.at[h * n_tp + tp], squares_in.at[tp * heads + h], own_sem.at[2 * h + 1]
            ),
        )

    order = list(range(2, n_tp)) + [1, 0]

    def phase_b(h, carry):
        lanes = lanes_of(h)
        for k in order:
            to = lax.rem(tp + k, n_tp)

            def block(j, _):
                sums = []
                for r in range(0, CHUNK, SUB):
                    first = j * CHUNK + r
                    at = pl.ds(pl.multiple_of(to * out_rows + first, SUB), SUB)
                    full = state[at, lanes] + prod[at, lanes] * carry
                    value = full * gate[at, lanes]
                    gated[h, at, :] = (value * out_gain[0:1, lanes]).astype(BF16)
                    square = value * value
                    part = square[:, 0:128]
                    for c in range(128, head, 128):
                        part = part + square[:, c : c + 128]
                    sums.append(part)
                row = jnp.sum(jnp.concatenate(sums, axis=0).T, axis=0, keepdims=True)
                squares[h * n_tp + to, :, pl.ds(pl.multiple_of(j * CHUNK, CHUNK), CHUNK)] = spread(row)
                return 0

            lax.fori_loop(0, out_rows // CHUNK, block, 0)
            if k == 0:
                for copy in own_copies(h):
                    copy.start()
            else:
                a_copy(h, k).start()
                q_copy(h, k).start()

    def wait_blocks(h):
        for copy in own_copies(h):
            copy.wait()
        for k in range(1, n_tp):
            a_copy(h, k).wait_recv()
            q_copy(h, k).wait_recv()

    def finish_w():
        for d in range(1, n_sp):
            c_copy(d, 0).wait_recv()
            c_copy(d, 1).wait_recv()

    tile = 512 if width % 512 == 0 else 256

    def multiply(h, columns):
        left = jnp.concatenate([arrived[k * heads + h] for k in range(n_tp)], axis=1)
        right = jnp.concatenate(
            [w_all[(k * heads + h) * head : (k * heads + h + 1) * head, columns] for k in range(n_tp)],
            axis=0,
        )
        return jnp.dot(left, right, preferred_element_type=F32)

    loads[0].wait()
    carry = start_carry()
    halo_copy.wait_recv()
    start_conv(0)
    loads[1].wait()
    carry = lax.fori_loop(0, chunks, lambda i, c: phase_a(0, i, c), carry)
    send_ends(0, carry)
    for d in far:
        z_copy(d).start()
    split = min(2, chunks)
    for h in range(1, heads):
        start_conv(h)
        carry = lax.fori_loop(0, split, functools.partial(phase_a, h), start_carry())
        phase_b(h - 1, take_ends(h - 1))
        if h == 1:
            forward_first(near)
        carry = lax.fori_loop(split, chunks, functools.partial(phase_a, h), carry)
        send_ends(h, carry)
    if heads == 1:
        forward_first(near)
    last = heads - 1
    phase_b(last, take_ends(last))
    forward_first(far)
    forward_second(near)
    forward_second(far)
    loads[2].wait()
    finish_w()
    for h in range(last):
        wait_blocks(h)

        def partial_sum(n, _, h=h):
            columns = pl.ds(pl.multiple_of(n * tile, tile), tile)
            value = multiply(h, columns)
            total[:, columns] = value if h == 0 else total[:, columns] + value
            return 0

        lax.fori_loop(0, width // tile, partial_sum, 0)
    wait_blocks(last)
    row = squares_in[0]
    for k in range(1, n_tp * heads):
        row = row + squares_in[k]
    out_scale = lax.rsqrt(row[0:1] / (n_tp * heads * head) + 1e-06)
    scale_cols = jnp.broadcast_to(out_scale, (128, out_rows)).T

    def out_copy(n):
        columns = pl.ds(pl.multiple_of(n * tile, tile), tile)
        return pltpu.make_async_copy(result.at[:, columns], out.at[:, columns], out_sem.at[n])

    def final(n, _):
        columns = pl.ds(pl.multiple_of(n * tile, tile), tile)
        value = multiply(last, columns)
        if last > 0:
            value = value + total[:, columns]
        value = value * jnp.concatenate([scale_cols] * (tile // 128), axis=1)
        result[:, columns] = value.astype(BF16)
        out_copy(n).start()
        return 0

    lax.fori_loop(0, width // tile, final, 0)

    halo_copy.wait_send()
    for d in range(1, n_sp):
        z_copy(d).wait_send()
        y_copy(d).wait_send()
        c_copy(d, 0).wait_send()
        c_copy(d, 1).wait_send()
        for h in range(heads):
            end_copy(h, d).wait_send()
    for h in range(heads):
        for k in range(1, n_tp):
            a_copy(h, k).wait_send()
            q_copy(h, k).wait_send()
    for n in range(width // tile):
        out_copy(n).wait()


def body(sizes, tokens, in_gain, w_input, w_gate, conv_taps, w_rate, w_inlet, decay_param,
         decay_bias, out_gain, w_out):
    n_grp, n_sp, n_tp = sizes
    rows, width = tokens.shape
    channels = w_input.shape[1]
    heads, head = w_rate.shape[0], w_rate.shape[1]
    out_rows = rows // n_tp
    out_width = w_out.shape[1]
    all_channels = channels * n_tp
    tile = 512 if out_width % 512 == 0 else 256
    rate_scale = (-8.0 * jax.nn.softplus(-decay_param)).reshape(1, channels)
    hbm = pl.BlockSpec(memory_space=pl.ANY)
    vmem = pl.BlockSpec(memory_space=pltpu.VMEM)
    dma = pltpu.SemaphoreType.DMA
    return pl.pallas_call(
        functools.partial(kernel, sizes),
        out_shape=jax.ShapeDtypeStruct((out_rows, out_width), BF16),
        in_specs=[hbm, vmem, hbm, hbm, vmem, vmem, vmem, vmem, vmem, vmem, hbm],
        out_specs=hbm,
        scratch_shapes=[
            pltpu.VMEM((rows, width), BF16),
            pltpu.VMEM((width, channels), BF16),
            pltpu.VMEM((width, channels), BF16),
            pltpu.VMEM((all_channels, out_width), BF16),
            pltpu.VMEM((rows, channels), F32),
            pltpu.VMEM((rows, channels), F32),
            pltpu.VMEM((rows, channels), F32),
            pltpu.VMEM((heads, rows, head), BF16),
            pltpu.VMEM((n_tp * heads, out_rows, head), BF16),
            pltpu.VMEM((out_rows, out_width), F32),
            pltpu.VMEM((out_rows, out_width), BF16),
            pltpu.VMEM((16, width), BF16),
            pltpu.VMEM((CHUNK + 8, head), F32),
            pltpu.VMEM((CHUNK, head), BF16),
            pltpu.VMEM((CHUNK, head), F32),
            pltpu.VMEM((CHUNK, head), F32),
            pltpu.VMEM((heads * n_tp, 8, out_rows), F32),
            pltpu.VMEM((n_tp * heads, 8, out_rows), F32),
            pltpu.VMEM((heads, 16, head), F32),
            pltpu.VMEM((heads * n_sp, 16, head), F32),
            dma((rows // CHUNK,)),
            dma((3,)),
            dma,
            dma,
            dma((n_sp,)),
            dma((n_sp,)),
            dma((n_sp,)),
            dma((n_sp,)),
            dma((2 * n_sp,)),
            dma((2 * n_sp,)),
            dma((heads * n_sp,)),
            dma((heads * n_sp,)),
            dma((heads * n_tp,)),
            dma((heads * n_tp,)),
            dma((heads * n_tp,)),
            dma((heads * n_tp,)),
            dma((2 * heads,)),
            dma((out_width // tile,)),
        ],
        compiler_params=pltpu.CompilerParams(
            collective_id=0, has_side_effects=True, vmem_limit_bytes=62 * 1024 * 1024
        ),
    )(
        tokens, in_gain.reshape(1, width), w_input, w_gate, conv_taps, w_rate, w_inlet,
        rate_scale, decay_bias, out_gain.reshape(1, channels), w_out,
    )


def solution(mesh):
    sizes = (mesh.shape["grp"], mesh.shape["sp"], mesh.shape["tp"])
    return jax.shard_map(
        functools.partial(body, sizes),
        mesh=mesh,
        in_specs=(
            P(("grp", "sp"), None),
            P(),
            P(None, "tp"),
            P(None, "tp"),
            P(None, "tp"),
            P("tp", None, None),
            P("tp", None, None),
            P("tp"),
            P("tp", ("grp", "sp")),
            P("tp"),
            P("sp", None),
        ),
        out_specs=P(("grp", "sp", "tp"), None),
        check_vma=False,
    )
```

```python
import functools
import jax
import jax.numpy as jnp
from jax import lax
from jax.experimental import pallas as pl
from jax.experimental.pallas import tpu as pltpu
from jax.sharding import PartitionSpec as P

MESH = pl.DeviceIdType.MESH
F32 = jnp.float32
BF16 = jnp.bfloat16
CHUNK = 256
SUB = 32


def normalize(raw, gain):
    as_float = raw.astype(F32)
    inv = lax.rsqrt(jnp.mean(as_float * as_float, axis=1, keepdims=True) + 1e-06)
    return (as_float * inv * gain).astype(BF16)


def one_minus_square(log_decay, decay):
    y = 2.0 * log_decay
    series = -y * (1.0 + y * (0.5 + y * (1.0 / 6 + y * (1.0 / 24 + y * (1.0 / 120)))))
    return jnp.where(y > -0.1, series, 1.0 - decay * decay)


def kernel(
    sizes,
    tokens, in_gain, w_input, w_gate, taps, w_rate, w_inlet, rate_scale, bias, out_gain, w_out,
    out,
    x, wi, wg, w_all, state, prod, gate, gated, arrived, total, result, halo, padded, conv,
    rate_in, inlet_in, squares, squares_in, ends, ends_in,
    x_sem, load_sem, halo_send, halo_recv, z_send, z_recv, x_send, x_recv, y_send, y_recv,
    c_send, c_recv,
    end_send, end_recv, a_send, a_recv, q_send, q_recv, own_sem, out_sem,
):
    n_grp, n_sp, n_tp = sizes
    grp, sp, tp = lax.axis_index("grp"), lax.axis_index("sp"), lax.axis_index("tp")
    rows, width = tokens.shape
    heads, head = w_rate.shape[0], w_rate.shape[1]
    reach = taps.shape[0] - 1
    chunks = rows // CHUNK
    out_rows = rows // n_tp
    shard = w_out.shape[0]
    piece = shard // (2 * n_grp * 2)
    core = lax.rem(tp, 2)
    mate = tp + 1 - 2 * core
    side = lax.rem(tp // 2, 2)
    beside = tp + 2 - 4 * side
    across = 1 - grp
    part = (core * n_grp + grp) * 2 + side
    part_beside = (core * n_grp + grp) * 2 + 1 - side

    def x_copy(i):
        at = pl.ds(pl.multiple_of(i * CHUNK, CHUNK), CHUNK)
        return pltpu.make_async_copy(tokens.at[at], x.at[at], x_sem.at[i])

    loads = [
        pltpu.make_async_copy(w_input, wi, load_sem.at[0]),
        pltpu.make_async_copy(w_gate, wg, load_sem.at[1]),
        pltpu.make_async_copy(
            w_out, w_all.at[pl.ds(pl.multiple_of(sp * shard, shard), shard)], load_sem.at[2]
        ),
    ]
    loads[0].start()
    x_copy(0).start()
    loads[1].start()
    for i in range(1, chunks):
        x_copy(i).start()
    loads[2].start()

    barrier = pltpu.get_barrier_semaphore()
    for d in range(1, n_sp):
        pl.semaphore_signal(
            barrier, inc=1, device_id={"sp": lax.rem(sp + d, n_sp)}, device_id_type=MESH
        )
    for k in range(1, n_tp):
        pl.semaphore_signal(
            barrier, inc=1, device_id={"tp": lax.rem(tp + k, n_tp)}, device_id_type=MESH
        )
    pl.semaphore_signal(barrier, inc=1, device_id={"grp": across}, device_id_type=MESH)
    pl.semaphore_wait(barrier, n_sp - 1 + n_tp - 1 + 1)

    def remote(src, dst, send, recv, where):
        return pltpu.make_async_remote_copy(
            src_ref=src, dst_ref=dst, send_sem=send, recv_sem=recv,
            device_id=where, device_id_type=MESH,
        )

    halo_rows = halo.shape[0]
    halo_copy = remote(
        tokens.at[pl.ds(rows - halo_rows, halo_rows)], halo, halo_send, halo_recv,
        {"sp": lax.rem(sp + 1, n_sp)},
    )
    halo_copy.start()

    def w_rows(d, which, count=1):
        source = lax.rem(sp + n_sp - d, n_sp)
        first = pl.multiple_of(source * shard + which * piece, piece)
        return w_all.at[pl.ds(first, count * piece)]

    def z_copy(d):
        return remote(
            w_out.at[pl.ds(pl.multiple_of(part * piece, piece), piece)],
            w_rows(0, part), z_send.at[d], z_recv.at[d], {"sp": lax.rem(sp + d, n_sp)},
        )

    def x_forward(d):
        at = w_rows(d, part)
        return remote(at, at, x_send.at[d], x_recv.at[d], {"tp": beside})

    def y_forward(d, second):
        at = w_rows(d, part_beside if second else part)
        k = 2 * d + second
        return remote(at, at, y_send.at[k], y_recv.at[k], {"grp": across})

    def c_forward(d):
        at = w_rows(d, core * n_grp * 2, n_grp * 2)
        return remote(at, at, c_send.at[d], c_recv.at[d], {"tp": mate})

    near = sorted({1, n_sp - 1})
    far = [d for d in range(2, n_sp - 1)]

    def forward_first(group):
        for d in group:
            z_copy(d).wait_recv()
            y_forward(d, 0).start()
            x_forward(d).start()

    def forward_second(group):
        for d in group:
            x_forward(d).wait_recv()
            y_forward(d, 1).start()

    def forward_third(group):
        for d in group:
            y_forward(d, 0).wait_recv()
            y_forward(d, 1).wait_recv()
            c_forward(d).start()

    def middle():
        forward_second(near)
        forward_first(far)

    head_last = heads - 1
    points = {(0, chunks - 3): lambda: forward_first(near)}
    points[(head_last, chunks - 2)] = lambda: forward_second(far)
    if heads == 1:
        points[(0, chunks - 2)] = middle
        points[(0, chunks - 1)] = lambda: forward_second(far)

    for d in near + far:
        z_copy(d).start()

    gain_row = in_gain[...]
    sublane = lax.broadcasted_iota(jnp.int32, (SUB // 8, 8, head), 1)

    def lanes_of(h):
        return slice(h * head, (h + 1) * head)

    def spread(row):
        return jnp.broadcast_to(row, (8, row.shape[1]))

    def start_conv(h):
        before = normalize(halo[...], gain_row)
        before = jnp.dot(before, wi[:, lanes_of(h)], preferred_element_type=F32)
        before = before.astype(BF16).astype(F32)
        padded[0:8, :] = jnp.where(sp > 0, before[halo_rows - 8 :], 0.0)

    def phase_a(h, i, carry):
        lanes = lanes_of(h)
        at = pl.ds(pl.multiple_of(i * CHUNK, CHUNK), CHUNK)
        for (point_head, point), action in points.items():
            if point_head == h:
                pl.when(i == point)(action)
        if h == 0:
            x_copy(i).wait()
            x[at, :] = normalize(x[at, :], gain_row)
        normed = x[at, :]
        projected = jnp.dot(normed, wi[:, lanes], preferred_element_type=F32)
        padded[8:, :] = projected.astype(BF16).astype(F32)
        for r in range(0, CHUNK, SUB):
            summed = padded[8 - reach + r : 8 - reach + r + SUB, :] * taps[0:1, lanes]
            for k in range(1, reach + 1):
                first = 8 - reach + k + r
                summed = summed + padded[first : first + SUB, :] * taps[k : k + 1, lanes]
            conv[r : r + SUB, :] = summed.astype(BF16)
        padded[0:8, :] = padded[CHUNK:, :]
        rate_in[...] = jnp.dot(conv[...], w_rate[h], preferred_element_type=F32)
        inlet_in[...] = jnp.dot(conv[...], w_inlet[h], preferred_element_type=F32)
        gate_raw = jnp.dot(normed, wg[:, lanes], preferred_element_type=F32)
        gate[at, lanes] = gate_raw
        bias_row = bias[h : h + 1, at]
        bias_cols = jnp.broadcast_to(bias_row, (128, CHUNK)).T
        scale = rate_scale[0:1, lanes]
        s, p = carry
        for r in range(0, CHUNK, SUB):
            here = slice(r, r + SUB)
            into = pl.ds(pl.multiple_of(i * CHUNK + r, SUB), SUB)
            raw = gate[into, lanes].astype(BF16).astype(F32)
            gate[into, lanes] = jax.nn.gelu(raw)
            bias_here = jnp.concatenate([bias_cols[here]] * (head // 128), axis=1)
            log_decay = jax.nn.sigmoid(rate_in[here, :]) * scale + bias_here
            decay = jnp.exp(log_decay)
            drive = (
                jnp.sqrt(one_minus_square(log_decay, decay))
                * jax.nn.sigmoid(inlet_in[here, :])
                * conv[here, :].astype(F32)
            )
            pt = decay.reshape(SUB // 8, 8, head)
            st = drive.reshape(SUB // 8, 8, head)
            for d in (1, 2, 4):
                inside = sublane >= d
                st = st + pt * jnp.where(inside, pltpu.roll(st, d, 1), 0.0)
                pt = pt * jnp.where(inside, pltpu.roll(pt, d, 1), 1.0)
            s_parts, p_parts = [], []
            for t in range(SUB // 8):
                s_parts.append(st[t] + pt[t] * s)
                p_parts.append(pt[t] * p)
                p_last = spread(pt[t, 7:8])
                s = spread(st[t, 7:8]) + p_last * s
                p = p_last * p
            state[into, lanes] = jnp.concatenate(s_parts, axis=0)
            prod[into, lanes] = jnp.concatenate(p_parts, axis=0)
        return s, p

    def start_carry():
        return jnp.zeros((8, head), F32), jnp.ones((8, head), F32)

    def end_copy(h, d):
        k = h * n_sp + d
        return remote(
            ends.at[h], ends_in.at[k], end_send.at[k], end_recv.at[k],
            {"sp": lax.rem(sp + d, n_sp)},
        )

    def send_ends(h, carry):
        s, p = carry
        ends[h, 0:8, :] = s
        ends[h, 8:16, :] = p
        for d in range(1, n_sp):
            end_copy(h, d).start()

    def take_ends(h):
        carry = jnp.zeros((8, head), F32)
        for d in range(n_sp - 1, 0, -1):
            end_copy(h, d).wait_recv()
            k = h * n_sp + d
            new = ends_in[k, 0:8, :] + ends_in[k, 8:16, :] * carry
            carry = jnp.where(d <= sp, new, carry)
        return carry[0:1]

    def a_copy(h, k):
        to = lax.rem(tp + k, n_tp)
        at = pl.ds(pl.multiple_of(to * out_rows, out_rows), out_rows)
        slot = h * n_tp + k
        return remote(
            gated.at[h, at], arrived.at[tp * heads + h], a_send.at[slot], a_recv.at[slot],
            {"tp": to},
        )

    def q_copy(h, k):
        to = lax.rem(tp + k, n_tp)
        slot = h * n_tp + k
        return remote(
            squares.at[h * n_tp + to], squares_in.at[tp * heads + h],
            q_send.at[slot], q_recv.at[slot], {"tp": to},
        )

    def own_copies(h):
        at = pl.ds(pl.multiple_of(tp * out_rows, out_rows), out_rows)
        return (
            pltpu.make_async_copy(gated.at[h, at], arrived.at[tp * heads + h], own_sem.at[2 * h]),
            pltpu.make_async_copy(
                squares.at[h * n_tp + tp], squares_in.at[tp * heads + h], own_sem.at[2 * h + 1]
            ),
        )

    order = list(range(2, n_tp)) + [1, 0]

    def phase_b(h, carry):
        lanes = lanes_of(h)
        for k in order:
            to = lax.rem(tp + k, n_tp)

            def block(j, _):
                sums = []
                for r in range(0, CHUNK, SUB):
                    first = j * CHUNK + r
                    at = pl.ds(pl.multiple_of(to * out_rows + first, SUB), SUB)
                    full = state[at, lanes] + prod[at, lanes] * carry
                    value = full * gate[at, lanes]
                    gated[h, at, :] = (value * out_gain[0:1, lanes]).astype(BF16)
                    square = value * value
                    part = square[:, 0:128]
                    for c in range(128, head, 128):
                        part = part + square[:, c : c + 128]
                    sums.append(part)
                row = jnp.sum(jnp.concatenate(sums, axis=0).T, axis=0, keepdims=True)
                squares[h * n_tp + to, :, pl.ds(pl.multiple_of(j * CHUNK, CHUNK), CHUNK)] = spread(row)
                return 0

            lax.fori_loop(0, out_rows // CHUNK, block, 0)
            if k == 0:
                for copy in own_copies(h):
                    copy.start()
            else:
                a_copy(h, k).start()
                q_copy(h, k).start()

    def wait_blocks(h):
        for copy in own_copies(h):
            copy.wait()
        for k in range(1, n_tp):
            a_copy(h, k).wait_recv()
            q_copy(h, k).wait_recv()

    def finish_w():
        for d in range(1, n_sp):
            c_forward(d).wait_recv()

    tile = 512 if width % 512 == 0 else 256

    def multiply(h, columns):
        left = jnp.concatenate([arrived[k * heads + h] for k in range(n_tp)], axis=1)
        right = jnp.concatenate(
            [w_all[(k * heads + h) * head : (k * heads + h + 1) * head, columns] for k in range(n_tp)],
            axis=0,
        )
        return jnp.dot(left, right, preferred_element_type=F32)

    loads[0].wait()
    carry = start_carry()
    halo_copy.wait_recv()
    start_conv(0)
    loads[1].wait()
    carry = lax.fori_loop(0, chunks, functools.partial(phase_a, 0), carry)
    send_ends(0, carry)
    split = min(2, chunks)
    for h in range(1, heads):
        start_conv(h)
        carry = lax.fori_loop(0, split, functools.partial(phase_a, h), start_carry())
        if h == 1:
            middle()
        phase_b(h - 1, take_ends(h - 1))
        carry = lax.fori_loop(split, chunks, functools.partial(phase_a, h), carry)
        send_ends(h, carry)
    last = heads - 1
    phase_b(last, take_ends(last))
    forward_third(near)
    forward_third(far)
    loads[2].wait()
    finish_w()
    for h in range(last):
        wait_blocks(h)

        def partial_sum(n, _, h=h):
            columns = pl.ds(pl.multiple_of(n * tile, tile), tile)
            value = multiply(h, columns)
            total[:, columns] = value if h == 0 else total[:, columns] + value
            return 0

        lax.fori_loop(0, width // tile, partial_sum, 0)
    wait_blocks(last)
    row = squares_in[0]
    for k in range(1, n_tp * heads):
        row = row + squares_in[k]
    out_scale = lax.rsqrt(row[0:1] / (n_tp * heads * head) + 1e-06)
    scale_cols = jnp.broadcast_to(out_scale, (128, out_rows)).T

    def out_copy(n):
        columns = pl.ds(pl.multiple_of(n * tile, tile), tile)
        return pltpu.make_async_copy(result.at[:, columns], out.at[:, columns], out_sem.at[n])

    def final(n, _):
        columns = pl.ds(pl.multiple_of(n * tile, tile), tile)
        value = multiply(last, columns)
        if last > 0:
            value = value + total[:, columns]
        value = value * jnp.concatenate([scale_cols] * (tile // 128), axis=1)
        result[:, columns] = value.astype(BF16)
        out_copy(n).start()
        return 0

    lax.fori_loop(0, width // tile, final, 0)

    halo_copy.wait_send()
    for d in range(1, n_sp):
        z_copy(d).wait_send()
        x_forward(d).wait_send()
        y_forward(d, 0).wait_send()
        y_forward(d, 1).wait_send()
        c_forward(d).wait_send()
        for h in range(heads):
            end_copy(h, d).wait_send()
    for h in range(heads):
        for k in range(1, n_tp):
            a_copy(h, k).wait_send()
            q_copy(h, k).wait_send()
    for n in range(width // tile):
        out_copy(n).wait()


def body(sizes, tokens, in_gain, w_input, w_gate, conv_taps, w_rate, w_inlet, decay_param,
         decay_bias, out_gain, w_out):
    n_grp, n_sp, n_tp = sizes
    rows, width = tokens.shape
    channels = w_input.shape[1]
    heads, head = w_rate.shape[0], w_rate.shape[1]
    out_rows = rows // n_tp
    out_width = w_out.shape[1]
    all_channels = channels * n_tp
    tile = 512 if out_width % 512 == 0 else 256
    rate_scale = (-8.0 * jax.nn.softplus(-decay_param)).reshape(1, channels)
    hbm = pl.BlockSpec(memory_space=pl.ANY)
    vmem = pl.BlockSpec(memory_space=pltpu.VMEM)
    dma = pltpu.SemaphoreType.DMA
    return pl.pallas_call(
        functools.partial(kernel, sizes),
        out_shape=jax.ShapeDtypeStruct((out_rows, out_width), BF16),
        in_specs=[hbm, vmem, hbm, hbm, vmem, vmem, vmem, vmem, vmem, vmem, hbm],
        out_specs=hbm,
        scratch_shapes=[
            pltpu.VMEM((rows, width), BF16),
            pltpu.VMEM((width, channels), BF16),
            pltpu.VMEM((width, channels), BF16),
            pltpu.VMEM((all_channels, out_width), BF16),
            pltpu.VMEM((rows, channels), F32),
            pltpu.VMEM((rows, channels), F32),
            pltpu.VMEM((rows, channels), F32),
            pltpu.VMEM((heads, rows, head), BF16),
            pltpu.VMEM((n_tp * heads, out_rows, head), BF16),
            pltpu.VMEM((out_rows, out_width), F32),
            pltpu.VMEM((out_rows, out_width), BF16),
            pltpu.VMEM((16, width), BF16),
            pltpu.VMEM((CHUNK + 8, head), F32),
            pltpu.VMEM((CHUNK, head), BF16),
            pltpu.VMEM((CHUNK, head), F32),
            pltpu.VMEM((CHUNK, head), F32),
            pltpu.VMEM((heads * n_tp, 8, out_rows), F32),
            pltpu.VMEM((n_tp * heads, 8, out_rows), F32),
            pltpu.VMEM((heads, 16, head), F32),
            pltpu.VMEM((heads * n_sp, 16, head), F32),
            dma((rows // CHUNK,)),
            dma((3,)),
            dma,
            dma,
            dma((n_sp,)),
            dma((n_sp,)),
            dma((n_sp,)),
            dma((n_sp,)),
            dma((2 * n_sp,)),
            dma((2 * n_sp,)),
            dma((n_sp,)),
            dma((n_sp,)),
            dma((heads * n_sp,)),
            dma((heads * n_sp,)),
            dma((heads * n_tp,)),
            dma((heads * n_tp,)),
            dma((heads * n_tp,)),
            dma((heads * n_tp,)),
            dma((2 * heads,)),
            dma((out_width // tile,)),
        ],
        compiler_params=pltpu.CompilerParams(
            collective_id=0, has_side_effects=True, vmem_limit_bytes=62 * 1024 * 1024
        ),
    )(
        tokens, in_gain.reshape(1, width), w_input, w_gate, conv_taps, w_rate, w_inlet,
        rate_scale, decay_bias, out_gain.reshape(1, channels), w_out,
    )


def solution(mesh):
    sizes = (mesh.shape["grp"], mesh.shape["sp"], mesh.shape["tp"])
    return jax.shard_map(
        functools.partial(body, sizes),
        mesh=mesh,
        in_specs=(
            P(("grp", "sp"), None),
            P(),
            P(None, "tp"),
            P(None, "tp"),
            P(None, "tp"),
            P("tp", None, None),
            P("tp", None, None),
            P("tp"),
            P("tp", ("grp", "sp")),
            P("tp"),
            P("sp", None),
        ),
        out_specs=P(("grp", "sp", "tp"), None),
        check_vma=False,
    )
```

```python
import functools
import math
import jax
import jax.numpy as jnp
from jax import lax
from jax.experimental import pallas as pl
from jax.experimental.pallas import tpu as pltpu
from jax.sharding import PartitionSpec as P

MESH = pl.DeviceIdType.MESH
F32 = jnp.float32
BF16 = jnp.bfloat16
CHUNK = 256
SUB = 32


def normalize(raw, gain):
    as_float = raw.astype(F32)
    inv = lax.rsqrt(jnp.mean(as_float * as_float, axis=1, keepdims=True) + 1e-06)
    return (as_float * inv * gain).astype(BF16)


LN4 = 2.0 * math.log(2.0)
GELU_A = math.sqrt(2.0 / math.pi)
GELU_B = GELU_A * 0.044715


def one_minus_square(log2_decay, decay):
    a1, a2, a3, a4 = -LN4, -(LN4**2) / 2, -(LN4**3) / 6, -(LN4**4) / 24
    series = log2_decay * (a1 + log2_decay * (a2 + log2_decay * (a3 + log2_decay * a4)))
    return jnp.where(log2_decay > -0.025, series, 1.0 - decay * decay)


def gelu_half(value):
    inner = value * (GELU_A + GELU_B * (value * value))
    return (0.25 * value) * (1.0 + jnp.tanh(inner))


def kernel(
    sizes,
    tokens, in_gain, w_input, w_gate, taps, w_rate, w_inlet, rate_scale, bias, out_gain, w_out,
    out,
    x, wi, wg, w_all, state, prod, gate, gated, arrived, total, result, halo, padded, conv,
    halved, rate_in, inlet_in, squares, squares_in, ends, ends_in,
    x_sem, load_sem, halo_send, halo_recv, z_send, z_recv, x_send, x_recv, y_send, y_recv,
    c_send, c_recv,
    end_send, end_recv, a_send, a_recv, q_send, q_recv, own_sem, out_sem,
):
    n_grp, n_sp, n_tp = sizes
    grp, sp, tp = lax.axis_index("grp"), lax.axis_index("sp"), lax.axis_index("tp")
    rows, width = tokens.shape
    heads, head = w_rate.shape[0], w_rate.shape[1]
    reach = taps.shape[0] - 1
    chunks = rows // CHUNK
    out_rows = rows // n_tp
    shard = w_out.shape[0]
    piece = shard // (2 * n_grp * 2)
    core = lax.rem(tp, 2)
    mate = tp + 1 - 2 * core
    side = lax.rem(tp // 2, 2)
    beside = tp + 2 - 4 * side
    across = 1 - grp
    part = (core * n_grp + grp) * 2 + side
    part_beside = (core * n_grp + grp) * 2 + 1 - side

    def x_copy(i):
        at = pl.ds(pl.multiple_of(i * CHUNK, CHUNK), CHUNK)
        return pltpu.make_async_copy(tokens.at[at], x.at[at], x_sem.at[i])

    loads = [
        pltpu.make_async_copy(w_input, wi, load_sem.at[0]),
        pltpu.make_async_copy(w_gate, wg, load_sem.at[1]),
        pltpu.make_async_copy(
            w_out, w_all.at[pl.ds(pl.multiple_of(sp * shard, shard), shard)], load_sem.at[2]
        ),
    ]
    loads[0].start()
    x_copy(0).start()
    loads[1].start()
    for i in range(1, chunks):
        x_copy(i).start()
    loads[2].start()

    barrier = pltpu.get_barrier_semaphore()
    for d in range(1, n_sp):
        pl.semaphore_signal(
            barrier, inc=1, device_id={"sp": lax.rem(sp + d, n_sp)}, device_id_type=MESH
        )
    for k in range(1, n_tp):
        pl.semaphore_signal(
            barrier, inc=1, device_id={"tp": lax.rem(tp + k, n_tp)}, device_id_type=MESH
        )
    pl.semaphore_signal(barrier, inc=1, device_id={"grp": across}, device_id_type=MESH)
    pl.semaphore_wait(barrier, n_sp - 1 + n_tp - 1 + 1)

    def remote(src, dst, send, recv, where):
        return pltpu.make_async_remote_copy(
            src_ref=src, dst_ref=dst, send_sem=send, recv_sem=recv,
            device_id=where, device_id_type=MESH,
        )

    halo_rows = halo.shape[0]
    halo_copy = remote(
        tokens.at[pl.ds(rows - halo_rows, halo_rows)], halo, halo_send, halo_recv,
        {"sp": lax.rem(sp + 1, n_sp)},
    )
    halo_copy.start()

    def w_rows(d, which, count=1):
        source = lax.rem(sp + n_sp - d, n_sp)
        first = pl.multiple_of(source * shard + which * piece, piece)
        return w_all.at[pl.ds(first, count * piece)]

    def z_copy(d):
        return remote(
            w_out.at[pl.ds(pl.multiple_of(part * piece, piece), piece)],
            w_rows(0, part), z_send.at[d], z_recv.at[d], {"sp": lax.rem(sp + d, n_sp)},
        )

    def x_forward(d):
        at = w_rows(d, part)
        return remote(at, at, x_send.at[d], x_recv.at[d], {"tp": beside})

    def y_forward(d, second):
        at = w_rows(d, part_beside if second else part)
        k = 2 * d + second
        return remote(at, at, y_send.at[k], y_recv.at[k], {"grp": across})

    def c_forward(d):
        at = w_rows(d, core * n_grp * 2, n_grp * 2)
        return remote(at, at, c_send.at[d], c_recv.at[d], {"tp": mate})

    near = sorted({1, n_sp - 1})
    far = [d for d in range(2, n_sp - 1)]

    def forward_first(group):
        for d in group:
            z_copy(d).wait_recv()
            y_forward(d, 0).start()
            x_forward(d).start()

    def forward_second(group):
        for d in group:
            x_forward(d).wait_recv()
            y_forward(d, 1).start()

    def forward_third(group):
        for d in group:
            y_forward(d, 0).wait_recv()
            y_forward(d, 1).wait_recv()
            c_forward(d).start()

    def middle():
        forward_second(near)
        forward_first(far)

    head_last = heads - 1
    points = {(0, chunks - 3): lambda: forward_first(near)}
    points[(head_last, chunks - 2)] = lambda: forward_second(far)
    if heads == 1:
        points[(0, chunks - 2)] = middle
        points[(0, chunks - 1)] = lambda: forward_second(far)

    for d in near + far:
        z_copy(d).start()

    gain_row = in_gain[...]
    sublane = lax.broadcasted_iota(jnp.int32, (SUB // 8, 8, head), 1)

    def lanes_of(h):
        return slice(h * head, (h + 1) * head)

    def spread(row):
        return jnp.broadcast_to(row, (8, row.shape[1]))

    def start_conv(h):
        before = normalize(halo[...], gain_row)
        before = jnp.dot(before, wi[:, lanes_of(h)], preferred_element_type=F32)
        padded[0:8, :] = jnp.where(sp > 0, before[halo_rows - 8 :], 0.0)

    def phase_a(h, i, carry):
        lanes = lanes_of(h)
        at = pl.ds(pl.multiple_of(i * CHUNK, CHUNK), CHUNK)
        for (point_head, point), action in points.items():
            if point_head == h:
                pl.when(i == point)(action)
        if h == 0:
            x_copy(i).wait()
            x[at, :] = normalize(x[at, :], gain_row)
        normed = x[at, :]
        projected = jnp.dot(normed, wi[:, lanes], preferred_element_type=F32)
        padded[8:, :] = projected
        for r in range(0, CHUNK, SUB):
            summed = padded[8 - reach + r : 8 - reach + r + SUB, :] * taps[0:1, lanes]
            for k in range(1, reach + 1):
                first = 8 - reach + k + r
                summed = summed + padded[first : first + SUB, :] * taps[k : k + 1, lanes]
            conv[r : r + SUB, :] = summed.astype(BF16)
        padded[0:8, :] = padded[CHUNK:, :]
        rate_in[...] = jnp.dot(conv[...], halved[2 * h], preferred_element_type=F32)
        inlet_in[...] = jnp.dot(conv[...], halved[2 * h + 1], preferred_element_type=F32)
        gate_raw = jnp.dot(normed, wg[:, lanes], preferred_element_type=F32)
        gate[at, lanes] = gelu_half(gate_raw)
        bias_row = bias[h : h + 1, at] * (1.0 / math.log(2.0))
        bias_cols = jnp.broadcast_to(bias_row, (128, CHUNK)).T
        scale = rate_scale[0:1, lanes]
        s, p = carry
        for r in range(0, CHUNK, SUB):
            here = slice(r, r + SUB)
            into = pl.ds(pl.multiple_of(i * CHUNK + r, SUB), SUB)
            bias_here = jnp.concatenate([bias_cols[here]] * (head // 128), axis=1)
            log2_decay = jnp.tanh(rate_in[here, :]) * scale + (bias_here + scale)
            decay = jnp.exp2(log2_decay)
            left = one_minus_square(log2_decay, decay)
            drive = (
                left * lax.rsqrt(jnp.maximum(left, 1e-37))
                * ((1.0 + jnp.tanh(inlet_in[here, :])) * conv[here, :].astype(F32))
            )
            pt = decay.reshape(SUB // 8, 8, head)
            st = drive.reshape(SUB // 8, 8, head)
            for d in (1, 2, 4):
                inside = sublane >= d
                st = st + pt * jnp.where(inside, pltpu.roll(st, d, 1), 0.0)
                pt = pt * jnp.where(inside, pltpu.roll(pt, d, 1), 1.0)
            s_parts, p_parts = [], []
            for t in range(SUB // 8):
                s_parts.append(st[t] + pt[t] * s)
                p_parts.append(pt[t] * p)
                p_last = spread(pt[t, 7:8])
                s = spread(st[t, 7:8]) + p_last * s
                p = p_last * p
            state[into, lanes] = jnp.concatenate(s_parts, axis=0)
            prod[into, lanes] = jnp.concatenate(p_parts, axis=0)
        return s, p

    def start_carry():
        return jnp.zeros((8, head), F32), jnp.ones((8, head), F32)

    def end_copy(h, d):
        k = h * n_sp + d
        return remote(
            ends.at[h], ends_in.at[k], end_send.at[k], end_recv.at[k],
            {"sp": lax.rem(sp + d, n_sp)},
        )

    def send_ends(h, carry):
        s, p = carry
        ends[h, 0:8, :] = s
        ends[h, 8:16, :] = p
        for d in range(1, n_sp):
            end_copy(h, d).start()

    def take_ends(h):
        carry = jnp.zeros((8, head), F32)
        for d in range(n_sp - 1, 0, -1):
            end_copy(h, d).wait_recv()
            k = h * n_sp + d
            new = ends_in[k, 0:8, :] + ends_in[k, 8:16, :] * carry
            carry = jnp.where(d <= sp, new, carry)
        return carry[0:1]

    def a_copy(h, k):
        to = lax.rem(tp + k, n_tp)
        at = pl.ds(pl.multiple_of(to * out_rows, out_rows), out_rows)
        slot = h * n_tp + k
        return remote(
            gated.at[h, at], arrived.at[tp * heads + h], a_send.at[slot], a_recv.at[slot],
            {"tp": to},
        )

    def q_copy(h, k):
        to = lax.rem(tp + k, n_tp)
        slot = h * n_tp + k
        return remote(
            squares.at[h * n_tp + to], squares_in.at[tp * heads + h],
            q_send.at[slot], q_recv.at[slot], {"tp": to},
        )

    def own_copies(h):
        at = pl.ds(pl.multiple_of(tp * out_rows, out_rows), out_rows)
        return (
            pltpu.make_async_copy(gated.at[h, at], arrived.at[tp * heads + h], own_sem.at[2 * h]),
            pltpu.make_async_copy(
                squares.at[h * n_tp + tp], squares_in.at[tp * heads + h], own_sem.at[2 * h + 1]
            ),
        )

    order = list(range(2, n_tp)) + [1, 0]

    def phase_b(h, carry):
        lanes = lanes_of(h)
        for k in order:
            to = lax.rem(tp + k, n_tp)

            def block(j, _):
                sums = []
                for r in range(0, CHUNK, SUB):
                    first = j * CHUNK + r
                    at = pl.ds(pl.multiple_of(to * out_rows + first, SUB), SUB)
                    full = state[at, lanes] + prod[at, lanes] * carry
                    value = full * gate[at, lanes]
                    gated[h, at, :] = (value * out_gain[0:1, lanes]).astype(BF16)
                    square = value * value
                    part = square[:, 0:128]
                    for c in range(128, head, 128):
                        part = part + square[:, c : c + 128]
                    sums.append(part)
                row = jnp.sum(jnp.concatenate(sums, axis=0).T, axis=0, keepdims=True)
                squares[h * n_tp + to, :, pl.ds(pl.multiple_of(j * CHUNK, CHUNK), CHUNK)] = spread(row)
                return 0

            lax.fori_loop(0, out_rows // CHUNK, block, 0)
            if k == 0:
                for copy in own_copies(h):
                    copy.start()
            else:
                a_copy(h, k).start()
                q_copy(h, k).start()

    def wait_blocks(h):
        for copy in own_copies(h):
            copy.wait()
        for k in range(1, n_tp):
            a_copy(h, k).wait_recv()
            q_copy(h, k).wait_recv()

    def finish_w():
        for d in range(1, n_sp):
            c_forward(d).wait_recv()

    tile = 512 if width % 512 == 0 else 256

    def multiply(h, columns):
        left = jnp.concatenate([arrived[k * heads + h] for k in range(n_tp)], axis=1)
        right = jnp.concatenate(
            [w_all[(k * heads + h) * head : (k * heads + h + 1) * head, columns] for k in range(n_tp)],
            axis=0,
        )
        return jnp.dot(left, right, preferred_element_type=F32)

    for h in range(heads):
        halved[2 * h] = w_rate[h] * 0.5
        halved[2 * h + 1] = w_inlet[h] * 0.5

    loads[0].wait()
    carry = start_carry()
    halo_copy.wait_recv()
    start_conv(0)
    loads[1].wait()
    carry = lax.fori_loop(0, chunks, functools.partial(phase_a, 0), carry)
    send_ends(0, carry)
    split = min(2, chunks)
    for h in range(1, heads):
        start_conv(h)
        carry = lax.fori_loop(0, split, functools.partial(phase_a, h), start_carry())
        if h == 1:
            middle()
        phase_b(h - 1, take_ends(h - 1))
        carry = lax.fori_loop(split, chunks, functools.partial(phase_a, h), carry)
        send_ends(h, carry)
    last = heads - 1
    phase_b(last, take_ends(last))
    forward_third(near)
    forward_third(far)
    loads[2].wait()
    finish_w()
    for h in range(last):
        wait_blocks(h)

        def partial_sum(n, _, h=h):
            columns = pl.ds(pl.multiple_of(n * tile, tile), tile)
            value = multiply(h, columns)
            total[:, columns] = value if h == 0 else total[:, columns] + value
            return 0

        lax.fori_loop(0, width // tile, partial_sum, 0)
    wait_blocks(last)
    row = squares_in[0]
    for k in range(1, n_tp * heads):
        row = row + squares_in[k]
    out_scale = lax.rsqrt(row[0:1] / (n_tp * heads * head) + 1e-06)
    scale_cols = jnp.broadcast_to(out_scale, (128, out_rows)).T

    def out_copy(n):
        columns = pl.ds(pl.multiple_of(n * tile, tile), tile)
        return pltpu.make_async_copy(result.at[:, columns], out.at[:, columns], out_sem.at[n])

    def final(n, _):
        columns = pl.ds(pl.multiple_of(n * tile, tile), tile)
        value = multiply(last, columns)
        if last > 0:
            value = value + total[:, columns]
        value = value * jnp.concatenate([scale_cols] * (tile // 128), axis=1)
        result[:, columns] = value.astype(BF16)
        out_copy(n).start()
        return 0

    lax.fori_loop(0, width // tile, final, 0)

    halo_copy.wait_send()
    for d in range(1, n_sp):
        z_copy(d).wait_send()
        x_forward(d).wait_send()
        y_forward(d, 0).wait_send()
        y_forward(d, 1).wait_send()
        c_forward(d).wait_send()
        for h in range(heads):
            end_copy(h, d).wait_send()
    for h in range(heads):
        for k in range(1, n_tp):
            a_copy(h, k).wait_send()
            q_copy(h, k).wait_send()
    for n in range(width // tile):
        out_copy(n).wait()


def body(sizes, tokens, in_gain, w_input, w_gate, conv_taps, w_rate, w_inlet, decay_param,
         decay_bias, out_gain, w_out):
    n_grp, n_sp, n_tp = sizes
    rows, width = tokens.shape
    channels = w_input.shape[1]
    heads, head = w_rate.shape[0], w_rate.shape[1]
    out_rows = rows // n_tp
    out_width = w_out.shape[1]
    all_channels = channels * n_tp
    tile = 512 if out_width % 512 == 0 else 256
    rate_scale = (-4.0 / math.log(2.0) * jax.nn.softplus(-decay_param)).reshape(1, channels)
    hbm = pl.BlockSpec(memory_space=pl.ANY)
    vmem = pl.BlockSpec(memory_space=pltpu.VMEM)
    dma = pltpu.SemaphoreType.DMA
    return pl.pallas_call(
        functools.partial(kernel, sizes),
        out_shape=jax.ShapeDtypeStruct((out_rows, out_width), BF16),
        in_specs=[hbm, vmem, hbm, hbm, vmem, vmem, vmem, vmem, vmem, vmem, hbm],
        out_specs=hbm,
        scratch_shapes=[
            pltpu.VMEM((rows, width), BF16),
            pltpu.VMEM((width, channels), BF16),
            pltpu.VMEM((width, channels), BF16),
            pltpu.VMEM((all_channels, out_width), BF16),
            pltpu.VMEM((rows, channels), F32),
            pltpu.VMEM((rows, channels), F32),
            pltpu.VMEM((rows, channels), F32),
            pltpu.VMEM((heads, rows, head), BF16),
            pltpu.VMEM((n_tp * heads, out_rows, head), BF16),
            pltpu.VMEM((out_rows, out_width), F32),
            pltpu.VMEM((out_rows, out_width), BF16),
            pltpu.VMEM((16, width), BF16),
            pltpu.VMEM((CHUNK + 8, head), F32),
            pltpu.VMEM((CHUNK, head), BF16),
            pltpu.VMEM((2 * heads, head, head), BF16),
            pltpu.VMEM((CHUNK, head), F32),
            pltpu.VMEM((CHUNK, head), F32),
            pltpu.VMEM((heads * n_tp, 8, out_rows), F32),
            pltpu.VMEM((n_tp * heads, 8, out_rows), F32),
            pltpu.VMEM((heads, 16, head), F32),
            pltpu.VMEM((heads * n_sp, 16, head), F32),
            dma((rows // CHUNK,)),
            dma((3,)),
            dma,
            dma,
            dma((n_sp,)),
            dma((n_sp,)),
            dma((n_sp,)),
            dma((n_sp,)),
            dma((2 * n_sp,)),
            dma((2 * n_sp,)),
            dma((n_sp,)),
            dma((n_sp,)),
            dma((heads * n_sp,)),
            dma((heads * n_sp,)),
            dma((heads * n_tp,)),
            dma((heads * n_tp,)),
            dma((heads * n_tp,)),
            dma((heads * n_tp,)),
            dma((2 * heads,)),
            dma((out_width // tile,)),
        ],
        compiler_params=pltpu.CompilerParams(
            collective_id=0, has_side_effects=True, vmem_limit_bytes=62 * 1024 * 1024
        ),
    )(
        tokens, in_gain.reshape(1, width), w_input, w_gate, conv_taps, w_rate, w_inlet,
        rate_scale, decay_bias, out_gain.reshape(1, channels), w_out,
    )


def solution(mesh):
    sizes = (mesh.shape["grp"], mesh.shape["sp"], mesh.shape["tp"])
    return jax.shard_map(
        functools.partial(body, sizes),
        mesh=mesh,
        in_specs=(
            P(("grp", "sp"), None),
            P(),
            P(None, "tp"),
            P(None, "tp"),
            P(None, "tp"),
            P("tp", None, None),
            P("tp", None, None),
            P("tp"),
            P("tp", ("grp", "sp")),
            P("tp"),
            P("sp", None),
        ),
        out_specs=P(("grp", "sp", "tp"), None),
        check_vma=False,
    )
```
